32 devices in a mesh: sp: 4 (over z), dp: 8 (over y, x, core).
Axes of the slice: x: 2, y: 2, z: 4, core: 2. Of those that a mesh axis runs over, the one named last changes fastest.
Arguments:
- cotangent: bfloat16 [8, 512, 2048], P('dp', 'sp'), may hold values from -6 to 6
- unit_pre: bfloat16 [8, 512, 2048], P('dp', None, 'sp'), may hold values from -6 to 6
- gate_pre: bfloat16 [8, 512, 2048], P('dp', None, 'sp'), may hold values from -15 to 15
- out_weight: bfloat16 [2048, 2048], P('dp', 'sp'), may hold values from -0.125 to 0.125
- mix_weight: bfloat16 [8, 128, 128], replicated, may hold values from -0.5 to 0.5
- mix_bias: bfloat16 [8, 128], replicated, may hold values from 0.099609375 to 1.8984375
- norm_gain: bfloat16 [2048], P('sp'), may hold values from 0.099609375 to 1.8984375
- norm_shift: bfloat16 [2048], P('sp'), may hold values from -3 to 3
Outputs:
- unit_grad: bfloat16 [8, 512, 2048], P('dp', None, 'sp')
- gate_grad: bfloat16 [8, 512, 2048], P('dp', None, 'sp')
- out_weight_grad: float32 [2048, 2048], P('dp', 'sp')
- mix_weight_grad: float32 [8, 128, 128], replicated
- mix_bias_grad: float32 [8, 128], replicated
- gain_grad: float32 [2048], P('sp')
- shift_grad: float32 [2048], P('sp')
The draws below stay inside these ranges and needn't reach their ends.
All inputs are finite; a program needn't handle non-finite values.
Results may differ from the reference program's by a relative error of at most 0.015.
Values may be sent and summed in bfloat16 or wider, within the bound.
No kernel may reach another device: no remote copies, remote signals or barrier semaphores. Data moves between devices by JAX's collectives and lax.ppermute only.
A program may use at most 64 MiB of HBM per device.

```python
import math
import jax
import jax.numpy as jnp
from jax import lax

D = 2048
GW = 2048
GROUPS = 8
BLK = 128
SEQ = 512
SEQS = 8


def draw_gate_pre(key, part):
    base = jax.random.fold_in(key, 11)
    noise_key, jitter_key = jax.random.split(base, 2)
    position = jnp.arange(GW).astype(jnp.float32) / GW
    jitter = jax.random.uniform(jitter_key, (GW,), jnp.float32, -0.3, 0.3)
    scales = jnp.exp(math.log(0.3) + position * math.log(10.0) + jitter)
    values = jnp.clip(jax.random.normal(noise_key, (SEQS, SEQ, GW), jnp.float32), -3.5, 3.5)
    return (values * scales).astype(jnp.bfloat16)


def block_scale(own_key, shape, shards, least, largest):
    factor_of = 1.0
    for dim, shards_of in shards:
        heights = jax.random.uniform(jax.random.fold_in(jax.random.fold_in(own_key, 6), dim), (shards_of,), jnp.float32, least / len(shards), largest / len(shards))
        factor_of = factor_of * jnp.repeat(jnp.exp(heights), shape[dim] // shards_of).reshape((-1,) + (1,) * (len(shape) - 1 - dim))
    return factor_of


def noise(own_key, extent, width, reach, shards=(), held_as=jnp.bfloat16):
    entries = width * jax.random.normal(own_key, extent, jnp.float32)
    if shards:
        entries = entries * block_scale(own_key, extent, shards, -0.22, 0.18)
    return jnp.clip(entries, -reach, reach).astype(held_as)


def setup_inputs(seed: int = 0) -> dict:
    streams_of = jax.random.split(jax.random.key(seed), 9)
    cotangent = noise(streams_of[0], (SEQS, SEQ, D), 1.0, 6.0, ((0, 8), (1, 4)))
    unit_pre = noise(streams_of[1], (SEQS, SEQ, GW), 1.0, 6.0, ((0, 8), (2, 4)))
    gate_pre = draw_gate_pre(jax.random.fold_in(streams_of[8], 71), 0)
    out_weight = noise(streams_of[3], (D, GW), GW ** -0.5, 0.125, ((0, 8), (1, 4)))
    mix_weight = noise(streams_of[4], (GROUPS, BLK, BLK), BLK ** -0.5, 0.5)
    mix_bias = jnp.clip(1.0 + 0.18 * jax.random.normal(streams_of[5], (GROUPS, BLK), jnp.float32), 0.099609375, 1.8984375).astype(jnp.bfloat16)
    norm_gain = jnp.clip(1.0 + 0.18 * jax.random.normal(streams_of[6], (GW,), jnp.float32), 0.099609375, 1.8984375).astype(jnp.bfloat16)
    norm_shift = noise(streams_of[7], (GW,), 0.5, 3.0, ((0, 4),))
    return {"cotangent": cotangent, "unit_pre": unit_pre, "gate_pre": gate_pre, "out_weight": out_weight, "mix_weight": mix_weight, "mix_bias": mix_bias, "norm_gain": norm_gain, "norm_shift": norm_shift}


epsilon = 1e-05
tanh_coef = math.sqrt(2.0 / math.pi)

def gelu_slope(values):
    inner = tanh_coef * (values + 0.044715 * values * values * values)
    hyper = jnp.tanh(inner)
    return 0.5 * (1.0 + hyper) + 0.5 * values * (1.0 - hyper * hyper) * tanh_coef * (1.0 + 3.0 * 0.044715 * values * values)

def reference(cotangent, unit_pre, gate_pre, out_weight, mix_weight, mix_bias, norm_gain, norm_shift):
    gdim = GW // GROUPS
    blocks = SEQ // BLK
    causal = jnp.arange(BLK)[:, None] >= jnp.arange(BLK)[None, :]
    masked = jnp.where(causal[None], mix_weight.astype(jnp.float32), jnp.float32(0.0))
    bias_full = mix_bias.astype(jnp.float32)
    gain_vec = norm_gain.astype(jnp.float32)
    shift_vec = norm_shift.astype(jnp.float32)

    def one_sequence(totals, inputs):
        dy_seq, unit_seq, gate_seq = inputs
        units = unit_seq.astype(jnp.float32)
        gates = gate_seq.astype(jnp.float32)
        unit_act = jax.nn.gelu(units)
        gate_act = jax.nn.gelu(gates)
        mean_val = lax.optimization_barrier(jnp.mean(gate_act, axis=-1))
        var_val = lax.optimization_barrier(jnp.mean(gate_act * gate_act, axis=-1)) - mean_val * mean_val
        rstd_val = lax.rsqrt(var_val + epsilon)
        centred = (gate_act - mean_val[:, None]) * rstd_val[:, None]
        normed = (centred * gain_vec + shift_vec).astype(jnp.bfloat16)
        normed_blocks = normed.astype(jnp.float32).reshape(blocks, BLK, GROUPS, gdim)
        mixed = jnp.einsum('gts,nsgd->ntgd', masked, normed_blocks) + bias_full.T[None, :, :, None]
        mixed = mixed.reshape(SEQ, GW)
        gated = (unit_act * mixed).astype(jnp.bfloat16)
        head_grad = jnp.dot(dy_seq, out_weight, preferred_element_type=jnp.float32)
        weight_term = lax.dot_general(dy_seq, gated, (((0,), (0,)), ((), ())), preferred_element_type=jnp.float32)
        unit_grad = (head_grad * mixed * gelu_slope(units)).astype(jnp.bfloat16)
        mix_grad = head_grad * unit_act
        mix_round = mix_grad.astype(jnp.bfloat16).astype(jnp.float32).reshape(blocks, BLK, GROUPS, gdim)
        mix_term = jnp.einsum('ntgd,nsgd->gts', mix_round, normed_blocks)
        mix_term = jnp.where(causal[None], mix_term, jnp.float32(0.0))
        bias_term = lax.optimization_barrier(jnp.sum(mix_grad.reshape(blocks, BLK, GROUPS, gdim), axis=(0, 3))).T
        normed_grad = jnp.einsum('gts,ntgd->nsgd', masked, mix_round).reshape(SEQ, GW)
        gain_term = lax.optimization_barrier(jnp.sum(normed_grad * centred, axis=0))
        shift_term = lax.optimization_barrier(jnp.sum(normed_grad, axis=0))
        scaled = normed_grad * gain_vec
        first_m = lax.optimization_barrier(jnp.mean(scaled, axis=-1))
        second_m = lax.optimization_barrier(jnp.mean(scaled * centred, axis=-1))
        gate_grad = (rstd_val[:, None] * (scaled - first_m[:, None] - centred * second_m[:, None]) * gelu_slope(gates)).astype(jnp.bfloat16)
        totals = (totals[0] + weight_term, totals[1] + mix_term, totals[2] + bias_term, totals[3] + gain_term, totals[4] + shift_term)
        return (totals, (unit_grad, gate_grad))
    start_totals = (jnp.zeros((D, GW), jnp.float32), jnp.zeros((GROUPS, BLK, BLK), jnp.float32), jnp.zeros((GROUPS, BLK), jnp.float32), jnp.zeros((GW,), jnp.float32), jnp.zeros((GW,), jnp.float32))
    totals, grads = lax.scan(one_sequence, start_totals, (cotangent, unit_pre, gate_pre))
    token_count = SEQS * SEQ
    norm_scale = 1.0 / math.sqrt(token_count)
    mix_scale = 1.0 / math.sqrt(token_count // BLK * gdim)
    return (grads[0], grads[1], totals[0] * norm_scale, totals[1] * mix_scale, totals[2] * mix_scale, totals[3] * norm_scale, totals[4] * norm_scale)
```

```python
import math

import jax
import jax.numpy as jnp
from jax import lax
from jax.sharding import PartitionSpec as P

GW = 2048
GROUPS = 8
BLK = 128

epsilon = 1e-05
tanh_coef = math.sqrt(2.0 / math.pi)
f32 = jnp.float32
bf16 = jnp.bfloat16


def gelu_both(values):
    inner = tanh_coef * (values + 0.044715 * values * values * values)
    hyper = jnp.tanh(inner)
    act = 0.5 * values * (1.0 + hyper)
    slope = 0.5 * (1.0 + hyper) + 0.5 * values * (1.0 - hyper * hyper) * tanh_coef * (
        1.0 + 3.0 * 0.044715 * values * values
    )
    return act, slope


def shift(value, step):
    count = lax.axis_size("sp")
    return lax.ppermute(value, "sp", [(i, (i + step) % count) for i in range(count)])


def swap(value, bit):
    count = lax.axis_size("dp")
    return lax.ppermute(value, "dp", [(i, i ^ (1 << bit)) for i in range(count)])


def bit_of(bit):
    return (lax.axis_index("dp") >> bit) & 1


def gather_bits(value, order):
    bits = len(order)
    full = value.reshape((1,) * bits + value.shape)
    for bit in order:
        axis = bits - 1 - bit
        other = swap(full, bit)
        mine = bit_of(bit) == 1
        full = jnp.where(
            mine,
            jnp.concatenate([other, full], axis),
            jnp.concatenate([full, other], axis),
        )
    return full


def halve(value, bit, bits):
    axis = bits - 1 - bit
    mine = bit_of(bit)
    send = lax.dynamic_slice_in_dim(value, 1 - mine, 1, axis).astype(bf16)
    keep = lax.dynamic_slice_in_dim(value, mine, 1, axis)
    return keep.astype(f32) + swap(send, bit).astype(f32)


def local(cotangent, unit_pre, gate_pre, out_weight, mix_weight, mix_bias, norm_gain, norm_shift):
    ring = lax.axis_size("sp")
    spot = lax.axis_index("sp")
    dps = lax.axis_size("dp")
    bits = dps.bit_length() - 1
    high_first = list(range(bits - 1, 0, -1)) + [0]
    low_first = list(range(1, bits)) + [0]
    seq_len = unit_pre.shape[1]
    channels = unit_pre.shape[2]
    rows = seq_len // ring
    per = rows // BLK
    blocks = seq_len // BLK
    group_dim = GW // GROUPS
    span = min(channels, group_dim)
    groups_here = channels // span
    group_start = spot * channels // group_dim

    dy = cotangent[0]
    width = dy.shape[1] // 2
    slots = [[dy[:, :width], dy[:, width:]]]
    for _ in range(ring - 1):
        slots.append([shift(part, 1) for part in slots[-1]])

    half = out_weight.shape[0] // 2
    top = gather_bits(out_weight[:half], high_first)
    low = gather_bits(out_weight[half:], low_first)
    weight = jnp.concatenate([top, low], axis=-2).reshape(dps * 2 * half, channels)
    weight_halves = [weight[:width], weight[width:]]

    def turned(value):
        return lax.dynamic_slice_in_dim(
            jnp.concatenate([value, value], 0), (spot + 1) * rows, seq_len, 0
        )

    units = turned(unit_pre[0]).astype(f32)
    gates = turned(gate_pre[0]).astype(f32)
    unit_act, unit_slope = gelu_both(units)
    gate_act, gate_slope = gelu_both(gates)

    def sum_sp(value, places):
        flat = places(value)
        total = flat
        for step in range(1, ring):
            total = total + shift(flat, step)
        return total

    def straight(value):
        return lax.dynamic_slice_in_dim(
            jnp.concatenate([value, value], 1), (ring - 1 - spot) * rows, seq_len, 1
        )

    def turn_back(value):
        return lax.dynamic_slice_in_dim(
            jnp.concatenate([value, value], 1), (spot + 1) * rows, seq_len, 1
        )

    moments = jnp.stack([jnp.sum(gate_act, axis=-1), jnp.sum(gate_act * gate_act, axis=-1)])
    moments = turn_back(sum_sp(moments, straight))
    mean_val = moments[0] / GW
    var_val = moments[1] / GW - mean_val * mean_val
    rstd_val = lax.rsqrt(var_val + epsilon)
    centred = (gate_act - mean_val[:, None]) * rstd_val[:, None]
    gain_vec = norm_gain.astype(f32)
    normed = (centred * gain_vec + norm_shift.astype(f32)).astype(bf16)
    causal = jnp.arange(BLK)[:, None] >= jnp.arange(BLK)[None, :]
    local_weight = lax.dynamic_slice_in_dim(mix_weight, group_start, groups_here, 0)
    masked = jnp.where(causal[None], local_weight, jnp.zeros_like(local_weight))
    local_bias = lax.dynamic_slice_in_dim(mix_bias, group_start, groups_here, 0).astype(f32)

    def per_block(weights, value, contract):
        count = value.shape[0] // BLK
        out = []
        for n in range(count):
            line = []
            for g in range(groups_here):
                piece = value[n * BLK : (n + 1) * BLK, g * span : (g + 1) * span]
                line.append(
                    lax.dot_general(
                        weights[g],
                        piece,
                        (((contract,), (0,)), ((), ())),
                        preferred_element_type=f32,
                    )
                )
            out.append(jnp.concatenate(line, 1))
        return jnp.concatenate(out, 0)

    bias_wide = jnp.concatenate(
        [jnp.broadcast_to(local_bias[g][:, None], (BLK, span)) for g in range(groups_here)], 1
    )
    mixed = per_block(masked, normed, 1) + jnp.tile(bias_wide, (blocks, 1))
    gated = (unit_act * mixed).astype(bf16)

    def stage(first, last):
        held = slice(first * rows, last * rows)
        picks = [slots[ring - 1 - p] for p in range(first, last)]
        sides = [jnp.concatenate([pick[c] for pick in picks], 0) for c in range(2)]
        product = sum(
            jnp.dot(side, wt, preferred_element_type=f32)
            for side, wt in zip(sides, weight_halves)
        )
        part = [
            lax.dot_general(
                side, gated[held], (((0,), (0,)), ((), ())), preferred_element_type=f32
            )
            for side in sides
        ]
        unit_grad = (product * mixed[held] * unit_slope[held]).astype(bf16)
        mix_grad = product * unit_act[held]
        mix_round = mix_grad.astype(bf16)
        mix_term = []
        bias_term = []
        for g in range(groups_here):
            lane = slice(g * span, (g + 1) * span)
            mix_term.append(
                sum(
                    lax.dot_general(
                        mix_round[n * BLK : (n + 1) * BLK, lane],
                        normed[held][n * BLK : (n + 1) * BLK, lane],
                        (((1,), (1,)), ((), ())),
                        preferred_element_type=f32,
                    )
                    for n in range((last - first) * per)
                )
            )
            bias_term.append(
                jnp.sum(
                    jnp.sum(mix_grad[:, lane], axis=1).reshape((last - first) * per, BLK), axis=0
                )
            )
        normed_grad = per_block(masked, mix_round, 0)
        gain_term = jnp.sum(normed_grad * centred[held], axis=0)
        shift_term = jnp.sum(normed_grad, axis=0)
        scaled = normed_grad * gain_vec
        sums = jnp.stack([jnp.sum(scaled, axis=-1), jnp.sum(scaled * centred[held], axis=-1)])
        return (
            part,
            unit_grad,
            (jnp.stack(mix_term), jnp.stack(bias_term), gain_term, shift_term),
            scaled,
            sums,
        )

    early = stage(1, ring)
    late = stage(0, 1)
    token_count = dps * seq_len
    norm_scale = 1.0 / math.sqrt(token_count)
    mix_scale = 1.0 / math.sqrt(token_count // BLK * group_dim)

    part = jnp.concatenate([a + b for a, b in zip(early[0], late[0])], 0)
    part = part.reshape((2,) * bits + (2 * half, channels))
    part = halve(part, 0, bits)
    pieces = []
    for side, order in ((part[..., :half, :], low_first), (part[..., half:, :], high_first)):
        for bit in order[:-1]:
            side = halve(side, bit, bits)
        pieces.append(side.reshape(half, channels))
    out_grad = jnp.concatenate(pieces, 0) * norm_scale

    back_sums = jnp.concatenate([late[4], early[4]], 1)
    back_sums = turn_back(sum_sp(back_sums, straight))
    first_m = back_sums[0] / GW
    second_m = back_sums[1] / GW
    scaled = jnp.concatenate([late[3], early[3]], 0)
    gate_grad = (
        rstd_val[:, None]
        * (scaled - first_m[:, None] - centred * second_m[:, None])
        * gate_slope
    ).astype(bf16)
    unit_grad = jnp.concatenate([late[1], early[1]], 0)

    def restored(value):
        return lax.dynamic_slice_in_dim(
            jnp.concatenate([value, value], 0), (ring - 1 - spot) * rows, seq_len, 0
        )

    mix_term, bias_term, gain_term, shift_term = (a + b for a, b in zip(early[2], late[2]))
    mix_term = jnp.where(causal[None], mix_term, f32(0.0))
    lanes = BLK
    chunks = [
        mix_term.reshape(-1, lanes),
        bias_term.reshape(-1, lanes),
        gain_term.reshape(-1, lanes),
        shift_term.reshape(-1, lanes),
    ]
    shared = groups_here * (BLK + 1)
    packed = jnp.concatenate(chunks, 0)
    for bit in [0] + list(range(1, bits)):
        sent = packed.astype(bf16)
        packed = sent.astype(f32) + swap(sent, bit).astype(f32)
    vecs = packed[shared:].reshape(2, channels) * norm_scale
    sent = packed[:shared].astype(bf16)
    every = [sent] + [shift(sent, step) for step in range(1, ring)]
    every = jnp.concatenate(every[::-1] * 2, 0)
    every = lax.dynamic_slice_in_dim(every, (ring - 1 - spot) * shared, ring * shared, 0)
    every = every.astype(f32).reshape(ring, shared, lanes)
    shares = max(1, ring * groups_here // GROUPS)
    full_weight = every[:, : groups_here * BLK].reshape(GROUPS, shares, BLK, BLK).sum(1)
    full_bias = every[:, groups_here * BLK :].reshape(GROUPS, shares, BLK).sum(1)
    return (
        restored(unit_grad)[None],
        restored(gate_grad)[None],
        out_grad,
        full_weight * mix_scale,
        full_bias * mix_scale,
        vecs[0],
        vecs[1],
    )


def solution(mesh):
    in_specs = (
        P("dp", "sp", None),
        P("dp", None, "sp"),
        P("dp", None, "sp"),
        P("dp", "sp"),
        P(),
        P(),
        P("sp"),
        P("sp"),
    )
    out_specs = (
        P("dp", None, "sp"),
        P("dp", None, "sp"),
        P("dp", "sp"),
        P(),
        P(),
        P("sp"),
        P("sp"),
    )
    return jax.shard_map(local, mesh=mesh, in_specs=in_specs, out_specs=out_specs, check_vma=False)
```
